32 devices in a mesh: grp: 2 (over y), fs: 4 (over z), tp: 4 (over x, core).
Axes of the slice: x: 2, y: 2, z: 4, core: 2. Of those that a mesh axis runs over, the one named last changes fastest.
Arguments:
- prompt: bfloat16 [2048, 2048], P(('grp', 'tp')), parts along dimension 0, may hold values from -6 to 6
- gain_first: float32 [2048], P('fs'), may hold values from 0.1 to 1.9
- gate_first: float32 [2048, 4096], P('fs', 'tp'), may hold values from -0.125 to 0.125
- up_first: float32 [2048, 4096], P('fs', 'tp'), may hold values from -0.125 to 0.125
- down_first: float32 [4096, 2048], P('fs', 'tp'), may hold values from -0.09375 to 0.09375
- gain_second: float32 [2048], P('fs'), may hold values from 0.1 to 1.9
- gate_second: float32 [2048, 4096], P('fs', 'tp'), may hold values from -0.125 to 0.125
- up_second: float32 [2048, 4096], P('fs', 'tp'), may hold values from -0.125 to 0.125
- down_second: float32 [4096, 2048], P('fs', 'tp'), may hold values from -0.09375 to 0.09375
Outputs:
- result: bfloat16 [2048, 2048], P(('grp', 'tp')), parts along dimension 0
- served_gate_first: bfloat16 [4096, 4096], P('grp', 'fs'), parts along dimension 0
- served_up_first: bfloat16 [4096, 4096], P('grp', 'fs'), parts along dimension 0
- served_down_first: bfloat16 [4096, 4096], P('fs', 'grp'), parts along dimension 1
- served_gate_second: bfloat16 [4096, 4096], P('grp', 'fs'), parts along dimension 0
- served_up_second: bfloat16 [4096, 4096], P('grp', 'fs'), parts along dimension 0
- served_down_second: bfloat16 [4096, 4096], P('fs', 'grp'), parts along dimension 1
The draws below stay inside these ranges and needn't reach their ends.
There are 2 independent parts, one for each index of `grp`. The reference program is written for one: setup_inputs(seed, part) draws one part's arguments, and reference() takes and returns one part's arrays. A program takes and returns all parts, laid end to end along the dimension named above; an argument that names none is the same for every part. Nothing has to cross between parts.
All inputs are finite; a program needn't handle non-finite values.
Results may differ from the reference program's by a relative error of at most 0.0053.
Values may be sent and summed in bfloat16 or wider, within the bound.
A program may use at most 128 MiB of HBM per device.

```python
import jax
import jax.numpy as jnp
from jax import lax

D = 2048
FF = 4096
TOKENS = 1024


def block_scale(rng, extent, shards, low, top_value):
    factor_of, own = 1.0, jax.random.fold_in(rng, 6)
    for position, blocks in shards:
        draws = jnp.exp(jax.random.uniform(jax.random.fold_in(own, position), (blocks,), jnp.float32, low / len(shards), top_value / len(shards)))
        factor_of = factor_of * jnp.repeat(draws, extent[position] // blocks).reshape([-1 if axis == position else 1 for axis in range(len(extent))])
    return factor_of


def gaussian(stream_key, dims, deviation, most, pieces=(), dtype=jnp.bfloat16):
    entries = deviation * jax.random.normal(stream_key, dims, jnp.float32)
    if pieces:
        entries = entries * block_scale(stream_key, dims, pieces, -0.22, 0.18)
    return jnp.clip(entries, -most, most).astype(dtype)


def setup_inputs(seed: int = 0, part: int = 0) -> dict:
    splits = jax.random.split(jax.random.key(seed), 10)
    own_keys = jax.random.split(jax.random.fold_in(splits[9], part), 10)
    return {
        "prompt": gaussian(own_keys[0], (TOKENS, D), 1.0, 6.0, ((0, 4),)),
        "gain_first": jnp.clip(1.0 + 0.18 * jax.random.normal(splits[1], (D,), jnp.float32), 0.1, 1.9),
        "gate_first": gaussian(splits[2], (D, FF), D ** -0.5, 0.125, ((0, 4), (1, 4)), jnp.float32),
        "up_first": gaussian(splits[3], (D, FF), D ** -0.5, 0.125, ((0, 4), (1, 4)), jnp.float32),
        "down_first": gaussian(splits[4], (FF, D), FF ** -0.5, 0.09375, ((0, 4), (1, 4)), jnp.float32),
        "gain_second": jnp.clip(1.0 + 0.18 * jax.random.normal(splits[5], (D,), jnp.float32), 0.1, 1.9),
        "gate_second": gaussian(splits[6], (D, FF), D ** -0.5, 0.125, ((0, 4), (1, 4)), jnp.float32),
        "up_second": gaussian(splits[7], (D, FF), D ** -0.5, 0.125, ((0, 4), (1, 4)), jnp.float32),
        "down_second": gaussian(splits[8], (FF, D), FF ** -0.5, 0.09375, ((0, 4), (1, 4)), jnp.float32),
    }


EPS = 1e-06

def fold(gain, weight):
    return (gain[:, None] * weight).astype(jnp.bfloat16)

def normed_of(stream):
    return (stream * lax.rsqrt(lax.optimization_barrier(jnp.mean(stream * stream, axis=-1, keepdims=True)) + EPS)).astype(jnp.bfloat16)

def block(stream, w_gate, w_up, w_down):
    normed = normed_of(stream)
    gate = jnp.dot(normed, w_gate, preferred_element_type=jnp.float32)
    up_val = jnp.dot(normed, w_up, preferred_element_type=jnp.float32)
    hidden = (jax.nn.silu(gate) * up_val).astype(jnp.bfloat16)
    return stream + 0.5 * jnp.dot(hidden, w_down, preferred_element_type=jnp.float32)

def reference(prompt, gain_first, gate_first, up_first, down_first, gain_second, gate_second, up_second, down_second):
    g_one = fold(gain_first, gate_first)
    u_one = fold(gain_first, up_first)
    d_one = down_first.astype(jnp.bfloat16)
    g_two = fold(gain_second, gate_second)
    u_two = fold(gain_second, up_second)
    d_two = down_second.astype(jnp.bfloat16)
    stream = prompt.astype(jnp.float32)
    stream = block(stream, g_one, u_one, d_one)
    stream = block(stream, g_two, u_two, d_two)
    return (stream.astype(jnp.bfloat16), g_one, u_one, d_one, g_two, u_two, d_two)
```

```python
import functools

import jax
import jax.numpy as jnp
from jax import lax
from jax.experimental import pallas as pl
from jax.experimental.pallas import tpu as pltpu
from jax.sharding import PartitionSpec as P

EPS = 1e-06
MESH = pl.DeviceIdType.MESH


def fold(gain, weight):
    return (gain[:, None] * weight).astype(jnp.bfloat16)


def kernel(n_grp, n_fs, n_tp, *refs):
    prompt = refs[0]
    ins, in_down = refs[1:5], refs[5:7]
    out_result, outs, out_down = refs[7], refs[8:12], refs[12:14]
    served, served_down = refs[14:18], refs[18:20]
    stream, normed, hidden, part, landed, spread = refs[20:26]
    (z_send, z_recv, x_send, x_recv, y_send, y_recv, c_send, c_recv, own_sem,
     dx_send, dx_recv, dy_send, dy_recv, dc_send, dc_recv, down_own,
     rs_send, rs_recv, ag_send, ag_recv, out_sem) = refs[26:]

    g, f, t = lax.axis_index("grp"), lax.axis_index("fs"), lax.axis_index("tp")
    ratio = n_fs // n_tp
    chips = n_tp // 2
    home = f // ratio
    is_home = t == home
    is_lane = lax.rem(t, 2) == lax.rem(home, 2)
    partner = t + 1 - 2 * lax.rem(t, 2)

    def along_fs(o):
        return lax.rem(f + o, n_fs)

    def along_tp(dx):
        return lax.rem(t + 2 * dx, n_tp)

    def along_grp(dg):
        return lax.rem(g + dg, n_grp)

    barrier = pltpu.get_barrier_semaphore()
    peers = (
        [{"fs": along_fs(o)} for o in range(1, n_fs)]
        + [{"tp": along_tp(dx)} for dx in range(1, chips)]
        + [{"grp": along_grp(dg)} for dg in range(1, n_grp)]
        + [{"tp": partner}]
    )
    for peer in peers:
        pl.semaphore_signal(barrier, inc=1, device_id=peer, device_id_type=MESH)
    pl.semaphore_wait(barrier, len(peers))

    def remote(src, dst, send, recv, where):
        return pltpu.make_async_remote_copy(
            src_ref=src, dst_ref=dst, send_sem=send, recv_sem=recv,
            device_id=where, device_id_type=MESH,
        )

    def arrived(dst, sem):
        pltpu.make_async_copy(dst, dst, sem).wait()

    rows = ins[0].shape[0]
    share = rows // n_grp
    width = served[0].shape[1]
    d_rows = served_down[0].shape[0]
    d_share = d_rows // n_grp
    d_cols = in_down[0].shape[1]

    def piece(m, r, h):
        return served[m].at[pl.ds(pl.multiple_of(r * rows + h * share, share), share)]

    def z_copy(m, j):
        src = ins[m].at[pl.ds(pl.multiple_of(g * share, share), share), pl.ds(j * width, width)]
        return src, piece(m, f, g), t * ratio + j

    def z_start(m):
        for j in range(ratio):
            src, dst, to = z_copy(m, j)

            @pl.when(to != f)
            def _():
                remote(src, dst, z_send.at[m, j], z_recv.at[m, f], {"fs": to}).start()

            @pl.when(to == f)
            def _():
                pltpu.make_async_copy(src, dst, own_sem.at[m]).start()

    def x_copy(m, r, dx):
        ref = piece(m, r, g)
        return remote(ref, ref, x_send.at[m, r, dx - 1], x_recv.at[m, r], {"tp": along_tp(dx)})

    def y_copy(m, r, dg):
        ref = piece(m, r, g)
        return remote(ref, ref, y_send.at[m, r, dg - 1], y_recv.at[m, r, g], {"grp": along_grp(dg)})

    def c_copy(m, r, h):
        ref = piece(m, r, h)
        return remote(ref, ref, c_send.at[m, r, h], c_recv.at[m, r, h], {"tp": partner})

    def primary(m):
        @pl.when(is_lane)
        def _():
            @pl.loop(0, n_fs)
            def _(o):
                r = along_fs(o)

                @pl.when(is_home)
                def _():
                    @pl.when(o == 0)
                    def _():
                        arrived(piece(m, r, g), own_sem.at[m])

                    @pl.when(o != 0)
                    def _():
                        arrived(piece(m, r, g), z_recv.at[m, r])

                    for dx in range(1, chips):
                        x_copy(m, r, dx).start()

                @pl.when(jnp.logical_not(is_home))
                def _():
                    arrived(piece(m, r, g), x_recv.at[m, r])

                for dg in range(1, n_grp):
                    y_copy(m, r, dg).start()
                c_copy(m, r, g).start()

    def secondary(m):
        @pl.when(is_lane)
        def _():
            @pl.loop(0, n_fs)
            def _(o):
                r = along_fs(o)
                for dg in range(1, n_grp):
                    h = along_grp(dg)
                    arrived(piece(m, r, h), y_recv.at[m, r, h])
                    c_copy(m, r, h).start()

        @pl.when(jnp.logical_not(is_lane))
        def _():
            @pl.loop(0, n_fs)
            def _(r):
                for h in range(n_grp):
                    arrived(piece(m, r, h), c_recv.at[m, r, h])

        pltpu.make_async_copy(served[m], outs[m], out_sem.at[m]).start()

    def d_piece(k, s, h):
        return served_down[k].at[
            pl.ds(pl.multiple_of(h * d_share, d_share), d_share),
            pl.ds(pl.multiple_of(s * d_cols, d_cols), d_cols),
        ]

    def d_block(k, s):
        return served_down[k].at[:, pl.ds(pl.multiple_of(s * d_cols, d_cols), d_cols)]

    def dx_copy(k, dx):
        src = in_down[k].at[pl.ds(pl.multiple_of(g * d_share, d_share), d_share)]
        return remote(src, d_piece(k, t, g), dx_send.at[k, dx - 1], dx_recv.at[k, dx - 1], {"tp": along_tp(dx)})

    def dy_copy(k, dx, dg):
        ref = d_piece(k, lax.rem(t + n_tp - 2 * dx, n_tp), g)
        return remote(ref, ref, dy_send.at[k, dx - 1, dg - 1], dy_recv.at[k, dx - 1, dg - 1], {"grp": along_grp(dg)})

    def dc_own(k):
        return remote(in_down[k], d_block(k, t), dc_send.at[k, 0], dc_recv.at[k, 0], {"tp": partner})

    def dc_copy(k, dx):
        ref = d_block(k, lax.rem(t + n_tp - 2 * dx, n_tp))
        return remote(ref, ref, dc_send.at[k, dx], dc_recv.at[k, dx], {"tp": partner})

    def down_start(k):
        for dx in range(1, chips):
            dx_copy(k, dx).start()
        dc_own(k).start()
        pltpu.make_async_copy(in_down[k], d_block(k, t), down_own.at[k]).start()

    def down_primary(k):
        for dx in range(1, chips):
            source = lax.rem(t + n_tp - 2 * dx, n_tp)
            arrived(d_piece(k, source, g), dx_recv.at[k, dx - 1])
            for dg in range(1, n_grp):
                dy_copy(k, dx, dg).start()

    def down_secondary(k):
        for dx in range(1, chips):
            source = lax.rem(t + n_tp - 2 * dx, n_tp)
            for dg in range(1, n_grp):
                arrived(d_piece(k, source, lax.rem(g + n_grp - dg, n_grp)), dy_recv.at[k, dx - 1, dg - 1])
            dc_copy(k, dx).start()
        arrived(d_block(k, t), down_own.at[k])
        arrived(d_block(k, partner), dc_recv.at[k, 0])
        for dx in range(1, chips):
            arrived(d_block(k, lax.rem(partner + n_tp - 2 * dx, n_tp)), dc_recv.at[k, dx])
        pltpu.make_async_copy(served_down[k], out_down[k], out_sem.at[4 + k]).start()

    tokens, features = prompt.shape
    owned = tokens // n_fs
    slab = min(64, tokens)
    tile = min(256, width)
    wide = min(256, features)

    def rs_copy(k, o):
        to = along_fs(o)
        return remote(part.at[k, to], landed.at[k, f], rs_send.at[k, o - 1], rs_recv.at[k, f], {"fs": to})

    def ag_copy(k, o):
        return remote(spread.at[k, f], spread.at[k, f], ag_send.at[k, o - 1], ag_recv.at[k, f], {"fs": along_fs(o)})

    def multiply(k):
        w_gate, w_up, w_down = served[2 * k], served[2 * k + 1], served_down[k]

        @pl.loop(0, tokens // slab)
        def _(i):
            at = pl.ds(pl.multiple_of(i * slab, slab), slab)
            value = stream[at]
            scale = lax.rsqrt(jnp.mean(value * value, axis=-1, keepdims=True) + EPS)
            normed[at] = (value * scale).astype(jnp.bfloat16)

        @pl.loop(0, width // tile)
        def _(i):
            at = pl.ds(pl.multiple_of(i * tile, tile), tile)
            gate = jnp.dot(normed[...], w_gate[:, at], preferred_element_type=jnp.float32)
            up = jnp.dot(normed[...], w_up[:, at], preferred_element_type=jnp.float32)
            hidden[:, at] = (jax.nn.silu(gate) * up).astype(jnp.bfloat16)

    def project(k):
        w_down = served_down[k]

        @pl.loop(0, features // wide)
        def _(i):
            at = pl.ds(pl.multiple_of(i * wide, wide), wide)
            value = jnp.dot(hidden[...], w_down[:, at], preferred_element_type=jnp.float32)
            for to in range(n_fs):
                part[k, to, :, at] = value[to * owned : (to + 1) * owned].astype(jnp.bfloat16)

        for o in range(1, n_fs):
            rs_copy(k, o).start()

    def add_up(k, last):
        for o in range(1, n_fs):
            arrived(landed.at[k, along_fs(o)], rs_recv.at[k, along_fs(o)])
        mine = pl.ds(pl.multiple_of(f * owned, owned), owned)

        @pl.loop(0, features // wide)
        def _(i):
            at = pl.ds(pl.multiple_of(i * wide, wide), wide)
            total = part[k, f, :, at].astype(jnp.float32)
            for o in range(1, n_fs):
                total = total + landed[k, along_fs(o), :, at].astype(jnp.float32)
            total = 0.5 * total
            if last:
                total = stream[mine, at] + total
            spread[k, f, :, at] = total.astype(jnp.bfloat16)

        for o in range(1, n_fs):
            ag_copy(k, o).start()

    def collect(k):
        for o in range(1, n_fs):
            arrived(spread.at[k, along_fs(o)], ag_recv.at[k, along_fs(o)])

    for m in range(2):
        z_start(m)
    down_start(0)
    for m in range(2, 4):
        z_start(m)

    stream[...] = prompt[...].astype(jnp.float32)

    primary(0)
    primary(1)
    down_primary(0)
    secondary(0)
    secondary(1)
    down_start(1)
    multiply(0)
    down_secondary(0)
    project(0)
    primary(2)
    add_up(0, False)
    primary(3)
    down_primary(1)
    secondary(2)
    collect(0)
    for to in range(n_fs):
        at = pl.ds(to * owned, owned)
        stream[at] = stream[at] + spread[0, to].astype(jnp.float32)
    secondary(3)
    multiply(1)
    down_secondary(1)
    project(1)
    add_up(1, True)
    collect(1)
    result_copy = pltpu.make_async_copy(spread.at[1], out_result, out_sem.at[6])
    result_copy.start()

    for m in range(4):
        for j in range(ratio):
            src, dst, to = z_copy(m, j)

            @pl.when(to != f)
            def _():
                remote(src, dst, z_send.at[m, j], z_recv.at[m, f], {"fs": to}).wait_send()

        @pl.when(is_lane)
        def _():
            @pl.loop(0, n_fs)
            def _(r):
                @pl.when(is_home)
                def _():
                    for dx in range(1, chips):
                        x_copy(m, r, dx).wait_send()

                for dg in range(1, n_grp):
                    y_copy(m, r, dg).wait_send()
                for h in range(n_grp):
                    c_copy(m, r, h).wait_send()

        pltpu.make_async_copy(served[m], outs[m], out_sem.at[m]).wait()
    for k in range(2):
        dc_own(k).wait_send()
        for dx in range(1, chips):
            dx_copy(k, dx).wait_send()
            dc_copy(k, dx).wait_send()
            for dg in range(1, n_grp):
                dy_copy(k, dx, dg).wait_send()
        for o in range(1, n_fs):
            rs_copy(k, o).wait_send()
            ag_copy(k, o).wait_send()
        pltpu.make_async_copy(served_down[k], out_down[k], out_sem.at[4 + k]).wait()
    result_copy.wait()


def on_device(
    n_grp, n_fs, n_tp,
    prompt,
    gain_first,
    gate_first,
    up_first,
    down_first,
    gain_second,
    gate_second,
    up_second,
    down_second,
):
    own = (
        fold(gain_first, gate_first),
        fold(gain_first, up_first),
        fold(gain_second, gate_second),
        fold(gain_second, up_second),
        down_first.astype(jnp.bfloat16),
        down_second.astype(jnp.bfloat16),
    )
    tokens, features = prompt.shape
    width = gate_first.shape[1] * n_tp // n_fs
    d_rows = down_first.shape[0]
    owned = tokens // n_fs
    chips = n_tp // 2
    gate_shape, down_shape = (features, width), (d_rows, features)
    bf16 = functools.partial(jax.ShapeDtypeStruct, dtype=jnp.bfloat16)
    shapes = [(n_fs, owned, features)] + [gate_shape] * 4 + [down_shape] * 2
    other_x, other_g = max(chips - 1, 1), max(n_grp - 1, 1)
    sems = [
        (4, n_fs // n_tp), (4, n_fs), (4, n_fs, other_x), (4, n_fs), (4, n_fs, other_g),
        (4, n_fs, n_grp), (4, n_fs, n_grp), (4, n_fs, n_grp), (4,),
        (2, other_x), (2, other_x), (2, other_x, other_g), (2, other_x, other_g),
        (2, chips), (2, chips), (2,),
        (2, n_fs), (2, n_fs), (2, n_fs), (2, n_fs), (7,),
    ]
    result, g1, u1, g2, u2, d1, d2 = pl.pallas_call(
        functools.partial(kernel, n_grp, n_fs, n_tp),
        out_shape=[bf16(s) for s in shapes],
        in_specs=[pl.BlockSpec(memory_space=pltpu.VMEM)] + [pl.BlockSpec(memory_space=pl.ANY)] * 6,
        out_specs=[pl.BlockSpec(memory_space=pl.ANY)] * 7,
        scratch_shapes=[pltpu.VMEM(gate_shape, jnp.bfloat16)] * 4
        + [pltpu.VMEM(down_shape, jnp.bfloat16)] * 2
        + [
            pltpu.VMEM((tokens, features), jnp.float32),
            pltpu.VMEM((tokens, features), jnp.bfloat16),
            pltpu.VMEM((tokens, width), jnp.bfloat16),
            pltpu.VMEM((2, n_fs, owned, features), jnp.bfloat16),
            pltpu.VMEM((2, n_fs, owned, features), jnp.bfloat16),
            pltpu.VMEM((2, n_fs, owned, features), jnp.bfloat16),
        ]
        + [pltpu.SemaphoreType.DMA(s) for s in sems],
        compiler_params=pltpu.CompilerParams(
            collective_id=0, has_side_effects=True, vmem_limit_bytes=56 * 2**20
        ),
        name="serve",
    )(prompt, *own)
    return (result.reshape(tokens, features), g1, u1, d1, g2, u2, d2)


def solution(mesh):
    return jax.shard_map(
        functools.partial(on_device, mesh.shape["grp"], mesh.shape["fs"], mesh.shape["tp"]),
        mesh=mesh,
        in_specs=(
            P(("grp", "tp"), None),
            P("fs"),
            P("fs", "tp"),
            P("fs", "tp"),
            P("fs", "tp"),
            P("fs"),
            P("fs", "tp"),
            P("fs", "tp"),
            P("fs", "tp"),
        ),
        out_specs=(
            P(("grp", "tp"), None),
            P("grp", "fs"),
            P("grp", "fs"),
            P("fs", "grp"),
            P("grp", "fs"),
            P("grp", "fs"),
            P("fs", "grp"),
        ),
        check_vma=False,
    )
```

```python
import functools

import jax
import jax.numpy as jnp
from jax import lax
from jax.experimental import pallas as pl
from jax.experimental.pallas import tpu as pltpu
from jax.sharding import PartitionSpec as P

EPS = 1e-06
MESH = pl.DeviceIdType.MESH


def fold(gain, weight):
    return (gain[:, None] * weight).astype(jnp.bfloat16)


def kernel(n_grp, n_fs, n_tp, n_sub, *refs):
    prompt = refs[0]
    ins, in_down = refs[1:5], refs[5:7]
    out_result, outs, out_down = refs[7], refs[8:12], refs[12:14]
    served, served_down = refs[14:18], refs[18:20]
    stream, normed, hidden, part, landed, spread, stage = refs[20:27]
    (p_send, p_recv, r_send, z_send, z_recv, x_send, x_recv, y_send, y_recv, c_send, c_recv, own_sem,
     dx_send, dx_recv, dy_send, dy_recv, dc_send, dc_recv, down_own,
     rs_send, rs_recv, ag_send, ag_recv, out_sem) = refs[27:]

    g, f, t = lax.axis_index("grp"), lax.axis_index("fs"), lax.axis_index("tp")
    ratio = n_fs // n_tp
    chips = n_tp // 2
    home = f // ratio
    mine_sub = lax.rem(t + n_tp - home, n_tp) // 2
    carries = mine_sub < n_sub
    is_lane = lax.rem(t, 2) == lax.rem(home, 2)
    partner = t + 1 - 2 * lax.rem(t, 2)

    def along_fs(o):
        return lax.rem(f + o, n_fs)

    def along_tp(dx):
        return lax.rem(t + 2 * dx, n_tp)

    def along_grp(dg):
        return lax.rem(g + dg, n_grp)

    barrier = pltpu.get_barrier_semaphore()
    peers = (
        [{"fs": along_fs(o)} for o in range(1, n_fs)]
        + [{"tp": along_tp(dx)} for dx in range(1, chips)]
        + [{"grp": along_grp(dg)} for dg in range(1, n_grp)]
        + [{"tp": partner}]
    )
    for peer in peers:
        pl.semaphore_signal(barrier, inc=1, device_id=peer, device_id_type=MESH)
    pl.semaphore_wait(barrier, len(peers))

    def remote(src, dst, send, recv, where):
        return pltpu.make_async_remote_copy(
            src_ref=src, dst_ref=dst, send_sem=send, recv_sem=recv,
            device_id=where, device_id_type=MESH,
        )

    def arrived(dst, sem):
        pltpu.make_async_copy(dst, dst, sem).wait()

    rows = ins[0].shape[0]
    share = rows // n_grp
    sub = share // n_sub
    width = served[0].shape[1]
    d_rows = served_down[0].shape[0]
    d_share = d_rows // n_grp
    d_cols = in_down[0].shape[1]

    def piece(m, r, h, s):
        return served[m].at[pl.ds(pl.multiple_of(r * rows + h * share + s * sub, sub), sub)]

    def p_copy(m, s):
        src = ins[m].at[pl.ds(pl.multiple_of(g * share + s * sub, sub), sub)]
        return remote(src, stage.at[m, s - 1], p_send.at[m, s - 1], p_recv.at[m, s - 1], {"tp": along_tp(s)})

    def z_copy(m, s, j):
        columns = pl.ds(j * width, width)
        if s == 0:
            src = ins[m].at[pl.ds(pl.multiple_of(g * share, share), sub), columns]
            return src, piece(m, f, g, s), t * ratio + j
        source = lax.rem(t + n_tp - 2 * s, n_tp)
        return stage.at[m, s - 1, :, columns], piece(m, f, g, s), source * ratio + j

    def z_remote(m, s, j):
        src, dst, to = z_copy(m, s, j)
        send = z_send.at[m, j] if s == 0 else r_send.at[m, s - 1, j]
        return remote(src, dst, send, z_recv.at[m, f], {"fs": to})

    def z_start(m, s):
        for j in range(ratio):
            src, dst, to = z_copy(m, s, j)

            @pl.when(to != f)
            def _():
                z_remote(m, s, j).start()

            @pl.when(to == f)
            def _():
                pltpu.make_async_copy(src, dst, own_sem.at[m]).start()

    def relay(m):
        for s in range(1, n_sub):
            arrived(stage.at[m, s - 1], p_recv.at[m, s - 1])
            z_start(m, s)

    def x_copy(m, r, dx):
        ref = piece(m, r, g, mine_sub)
        return remote(ref, ref, x_send.at[m, r, dx - 1], x_recv.at[m, r, mine_sub], {"tp": along_tp(dx)})

    def y_copy(m, r, dg, s):
        ref = piece(m, r, g, s)
        return remote(ref, ref, y_send.at[m, r, dg - 1, s], y_recv.at[m, r, g, s], {"grp": along_grp(dg)})

    def c_copy(m, r, h, s):
        ref = piece(m, r, h, s)
        return remote(ref, ref, c_send.at[m, r, h, s], c_recv.at[m, r, h, s], {"tp": partner})

    def primary(m):
        @pl.when(is_lane)
        def _():
            @pl.loop(0, n_fs)
            def _(o):
                r = along_fs(o)

                @pl.when(carries)
                def _():
                    @pl.when(o == 0)
                    def _():
                        arrived(piece(m, r, g, mine_sub), own_sem.at[m])

                    @pl.when(o != 0)
                    def _():
                        arrived(piece(m, r, g, mine_sub), z_recv.at[m, r])

                    for dx in range(1, chips):
                        x_copy(m, r, dx).start()
                    for dg in range(1, n_grp):
                        y_copy(m, r, dg, mine_sub).start()
                    c_copy(m, r, g, mine_sub).start()

    def crossed(m):
        @pl.when(is_lane)
        def _():
            @pl.loop(0, n_fs)
            def _(o):
                r = along_fs(o)
                for s in range(n_sub):
                    @pl.when(mine_sub != s)
                    def _():
                        arrived(piece(m, r, g, s), x_recv.at[m, r, s])
                        for dg in range(1, n_grp):
                            y_copy(m, r, dg, s).start()
                        c_copy(m, r, g, s).start()

    def secondary(m):
        @pl.when(is_lane)
        def _():
            @pl.loop(0, n_fs)
            def _(o):
                r = along_fs(o)
                for dg in range(1, n_grp):
                    h = along_grp(dg)
                    for s in range(n_sub):
                        arrived(piece(m, r, h, s), y_recv.at[m, r, h, s])
                        c_copy(m, r, h, s).start()

        @pl.when(jnp.logical_not(is_lane))
        def _():
            @pl.loop(0, n_fs)
            def _(r):
                for h in range(n_grp):
                    for s in range(n_sub):
                        arrived(piece(m, r, h, s), c_recv.at[m, r, h, s])

        pltpu.make_async_copy(served[m], outs[m], out_sem.at[m]).start()

    def d_piece(k, s, h):
        return served_down[k].at[
            pl.ds(pl.multiple_of(h * d_share, d_share), d_share),
            pl.ds(pl.multiple_of(s * d_cols, d_cols), d_cols),
        ]

    def d_block(k, s):
        return served_down[k].at[:, pl.ds(pl.multiple_of(s * d_cols, d_cols), d_cols)]

    def dx_copy(k, dx):
        src = in_down[k].at[pl.ds(pl.multiple_of(g * d_share, d_share), d_share)]
        return remote(src, d_piece(k, t, g), dx_send.at[k, dx - 1], dx_recv.at[k, dx - 1], {"tp": along_tp(dx)})

    def dy_copy(k, dx, dg):
        ref = d_piece(k, lax.rem(t + n_tp - 2 * dx, n_tp), g)
        return remote(ref, ref, dy_send.at[k, dx - 1, dg - 1], dy_recv.at[k, dx - 1, dg - 1], {"grp": along_grp(dg)})

    def dc_own(k):
        return remote(in_down[k], d_block(k, t), dc_send.at[k, 0], dc_recv.at[k, 0], {"tp": partner})

    def dc_copy(k, dx):
        ref = d_block(k, lax.rem(t + n_tp - 2 * dx, n_tp))
        return remote(ref, ref, dc_send.at[k, dx], dc_recv.at[k, dx], {"tp": partner})

    def down_start(k):
        for dx in range(1, chips):
            dx_copy(k, dx).start()
        dc_own(k).start()
        pltpu.make_async_copy(in_down[k], d_block(k, t), down_own.at[k]).start()

    def down_primary(k):
        for dx in range(1, chips):
            source = lax.rem(t + n_tp - 2 * dx, n_tp)
            arrived(d_piece(k, source, g), dx_recv.at[k, dx - 1])
            for dg in range(1, n_grp):
                dy_copy(k, dx, dg).start()

    def down_secondary(k):
        for dx in range(1, chips):
            source = lax.rem(t + n_tp - 2 * dx, n_tp)
            for dg in range(1, n_grp):
                arrived(d_piece(k, source, lax.rem(g + n_grp - dg, n_grp)), dy_recv.at[k, dx - 1, dg - 1])
            dc_copy(k, dx).start()
        arrived(d_block(k, t), down_own.at[k])
        arrived(d_block(k, partner), dc_recv.at[k, 0])
        for dx in range(1, chips):
            arrived(d_block(k, lax.rem(partner + n_tp - 2 * dx, n_tp)), dc_recv.at[k, dx])
        pltpu.make_async_copy(served_down[k], out_down[k], out_sem.at[4 + k]).start()

    tokens, features = prompt.shape
    owned = tokens // n_fs
    slab = min(64, tokens)
    tile = min(256, width)
    wide = min(256, features)

    def rs_copy(k, o):
        to = along_fs(o)
        return remote(part.at[k, to], landed.at[k, f], rs_send.at[k, o - 1], rs_recv.at[k, f], {"fs": to})

    def ag_copy(k, o):
        return remote(spread.at[k, f], spread.at[k, f], ag_send.at[k, o - 1], ag_recv.at[k, f], {"fs": along_fs(o)})

    def multiply(k):
        w_gate, w_up, w_down = served[2 * k], served[2 * k + 1], served_down[k]

        @pl.loop(0, tokens // slab)
        def _(i):
            at = pl.ds(pl.multiple_of(i * slab, slab), slab)
            value = stream[at]
            scale = lax.rsqrt(jnp.mean(value * value, axis=-1, keepdims=True) + EPS)
            normed[at] = (value * scale).astype(jnp.bfloat16)

        @pl.loop(0, width // tile)
        def _(i):
            at = pl.ds(pl.multiple_of(i * tile, tile), tile)
            gate = jnp.dot(normed[...], w_gate[:, at], preferred_element_type=jnp.float32)
            up = jnp.dot(normed[...], w_up[:, at], preferred_element_type=jnp.float32)
            hidden[:, at] = (jax.nn.silu(gate) * up).astype(jnp.bfloat16)

    def project(k):
        w_down = served_down[k]

        @pl.loop(0, features // wide)
        def _(i):
            at = pl.ds(pl.multiple_of(i * wide, wide), wide)
            value = jnp.dot(hidden[...], w_down[:, at], preferred_element_type=jnp.float32)
            for to in range(n_fs):
                part[k, to, :, at] = value[to * owned : (to + 1) * owned].astype(jnp.bfloat16)

        for o in range(1, n_fs):
            rs_copy(k, o).start()

    def add_up(k, last):
        for o in range(1, n_fs):
            arrived(landed.at[k, along_fs(o)], rs_recv.at[k, along_fs(o)])
        mine = pl.ds(pl.multiple_of(f * owned, owned), owned)

        @pl.loop(0, features // wide)
        def _(i):
            at = pl.ds(pl.multiple_of(i * wide, wide), wide)
            total = part[k, f, :, at].astype(jnp.float32)
            for o in range(1, n_fs):
                total = total + landed[k, along_fs(o), :, at].astype(jnp.float32)
            total = 0.5 * total
            if last:
                total = stream[mine, at] + total
            spread[k, f, :, at] = total.astype(jnp.bfloat16)

        for o in range(1, n_fs):
            ag_copy(k, o).start()

    def collect(k):
        for o in range(1, n_fs):
            arrived(spread.at[k, along_fs(o)], ag_recv.at[k, along_fs(o)])

    for m in range(4):
        for s in range(1, n_sub):
            p_copy(m, s).start()
        z_start(m, 0)
        if m % 2 == 1:
            down_start(m // 2)

    stream[...] = prompt[...].astype(jnp.float32)

    relay(0)
    relay(1)
    primary(0)
    relay(2)
    primary(1)
    relay(3)
    crossed(0)
    primary(2)
    crossed(1)
    down_primary(0)
    primary(3)
    secondary(0)
    secondary(1)
    multiply(0)
    crossed(2)
    down_secondary(0)
    project(0)
    crossed(3)
    down_primary(1)
    secondary(2)
    add_up(0, False)
    secondary(3)
    collect(0)
    for to in range(n_fs):
        at = pl.ds(to * owned, owned)
        stream[at] = stream[at] + spread[0, to].astype(jnp.float32)
    multiply(1)
    down_secondary(1)
    project(1)
    add_up(1, True)
    collect(1)
    result_copy = pltpu.make_async_copy(spread.at[1], out_result, out_sem.at[6])
    result_copy.start()

    for m in range(4):
        for s in range(n_sub):
            if s > 0:
                p_copy(m, s).wait_send()
            for j in range(ratio):
                @pl.when(z_copy(m, s, j)[2] != f)
                def _():
                    z_remote(m, s, j).wait_send()

        @pl.when(is_lane)
        def _():
            @pl.loop(0, n_fs)
            def _(r):
                @pl.when(carries)
                def _():
                    for dx in range(1, chips):
                        x_copy(m, r, dx).wait_send()

                for s in range(n_sub):
                    for dg in range(1, n_grp):
                        y_copy(m, r, dg, s).wait_send()
                    for h in range(n_grp):
                        c_copy(m, r, h, s).wait_send()

        pltpu.make_async_copy(served[m], outs[m], out_sem.at[m]).wait()
    for k in range(2):
        dc_own(k).wait_send()
        for dx in range(1, chips):
            dx_copy(k, dx).wait_send()
            dc_copy(k, dx).wait_send()
            for dg in range(1, n_grp):
                dy_copy(k, dx, dg).wait_send()
        for o in range(1, n_fs):
            rs_copy(k, o).wait_send()
            ag_copy(k, o).wait_send()
        pltpu.make_async_copy(served_down[k], out_down[k], out_sem.at[4 + k]).wait()
    result_copy.wait()


def on_device(
    n_grp, n_fs, n_tp,
    prompt,
    gain_first,
    gate_first,
    up_first,
    down_first,
    gain_second,
    gate_second,
    up_second,
    down_second,
):
    own = (
        fold(gain_first, gate_first),
        fold(gain_first, up_first),
        fold(gain_second, gate_second),
        fold(gain_second, up_second),
        down_first.astype(jnp.bfloat16),
        down_second.astype(jnp.bfloat16),
    )
    tokens, features = prompt.shape
    width = gate_first.shape[1] * n_tp // n_fs
    d_rows = down_first.shape[0]
    owned = tokens // n_fs
    chips = n_tp // 2
    gate_shape, down_shape = (features, width), (d_rows, features)
    bf16 = functools.partial(jax.ShapeDtypeStruct, dtype=jnp.bfloat16)
    shapes = [(n_fs, owned, features)] + [gate_shape] * 4 + [down_shape] * 2
    share = gate_first.shape[0] // n_grp
    n_sub = chips if share % (16 * chips) == 0 else 1
    other_x, other_g = max(chips - 1, 1), max(n_grp - 1, 1)
    sems = [
        (4, other_x), (4, other_x), (4, other_x, n_fs // n_tp),
        (4, n_fs // n_tp), (4, n_fs), (4, n_fs, other_x), (4, n_fs, n_sub), (4, n_fs, other_g, n_sub),
        (4, n_fs, n_grp, n_sub), (4, n_fs, n_grp, n_sub), (4, n_fs, n_grp, n_sub), (4,),
        (2, other_x), (2, other_x), (2, other_x, other_g), (2, other_x, other_g),
        (2, chips), (2, chips), (2,),
        (2, n_fs), (2, n_fs), (2, n_fs), (2, n_fs), (7,),
    ]
    result, g1, u1, g2, u2, d1, d2 = pl.pallas_call(
        functools.partial(kernel, n_grp, n_fs, n_tp, n_sub),
        out_shape=[bf16(s) for s in shapes],
        in_specs=[pl.BlockSpec(memory_space=pltpu.VMEM)] + [pl.BlockSpec(memory_space=pl.ANY)] * 6,
        out_specs=[pl.BlockSpec(memory_space=pl.ANY)] * 7,
        scratch_shapes=[pltpu.VMEM(gate_shape, jnp.bfloat16)] * 4
        + [pltpu.VMEM(down_shape, jnp.bfloat16)] * 2
        + [
            pltpu.VMEM((tokens, features), jnp.float32),
            pltpu.VMEM((tokens, features), jnp.bfloat16),
            pltpu.VMEM((tokens, width), jnp.bfloat16),
            pltpu.VMEM((2, n_fs, owned, features), jnp.bfloat16),
            pltpu.VMEM((2, n_fs, owned, features), jnp.bfloat16),
            pltpu.VMEM((2, n_fs, owned, features), jnp.bfloat16),
            pltpu.VMEM((4, other_x, share // n_sub, gate_first.shape[1]), jnp.bfloat16),
        ]
        + [pltpu.SemaphoreType.DMA(s) for s in sems],
        compiler_params=pltpu.CompilerParams(
            collective_id=0, has_side_effects=True, vmem_limit_bytes=56 * 2**20
        ),
        name="serve",
    )(prompt, *own)
    return (result.reshape(tokens, features), g1, u1, d1, g2, u2, d2)


def solution(mesh):
    return jax.shard_map(
        functools.partial(on_device, mesh.shape["grp"], mesh.shape["fs"], mesh.shape["tp"]),
        mesh=mesh,
        in_specs=(
            P(("grp", "tp"), None),
            P("fs"),
            P("fs", "tp"),
            P("fs", "tp"),
            P("fs", "tp"),
            P("fs"),
            P("fs", "tp"),
            P("fs", "tp"),
            P("fs", "tp"),
        ),
        out_specs=(
            P(("grp", "tp"), None),
            P("grp", "fs"),
            P("grp", "fs"),
            P("fs", "grp"),
            P("grp", "fs"),
            P("grp", "fs"),
            P("fs", "grp"),
        ),
        check_vma=False,
    )
```
